32 devices in a mesh: grp: 2 (over x), ep: 16 (over z, y, core).
Axes of the slice: x: 2, y: 2, z: 4, core: 2. Of those that a mesh axis runs over, the one named last changes fastest.
Arguments:
- tokens: bfloat16 [4096, 2048], P(('grp', 'ep')), parts along dimension 0, may hold values from -6 to 6
- norm_gain: float32 [2048], replicated, may hold values from 0.1 to 1.9
- expert_ids: int32 [4096, 2], P(('grp', 'ep')), parts along dimension 0, may hold values from 0 to 3, as said below
- mix_weights: float32 [4096, 2], P(('grp', 'ep')), parts along dimension 0, may hold values from 0.2 to 1
- gate_weight: bfloat16 [2048, 28672], P(None, 'ep'), may hold values from -0.125 to 0.125
- up_weight: bfloat16 [2048, 28672], P(None, 'ep'), may hold values from -0.125 to 0.125
- down_weight: bfloat16 [28672, 2048], P('ep'), may hold values from -0.0625 to 0.0625
Outputs:
- mixed: bfloat16 [4096, 2048], P(('grp', 'ep')), parts along dimension 0
The draws below stay inside these ranges and needn't reach their ends.
There are 2 independent parts, one for each index of `grp`. The reference program is written for one: setup_inputs(seed, part) draws one part's arguments, and reference() takes and returns one part's arrays. A program takes and returns all parts, laid end to end along the dimension named above; an argument that names none is the same for every part. Nothing has to cross between parts.
Inputs may be any that keep to these rules, and one draw needn't show every extreme that they name: `expert_ids`: each token names 2 different experts. In the rows of one device no expert is named by more than 80 rows, and in every draw each expert is named by exactly 80 rows of some device.
All inputs are finite; a program needn't handle non-finite values.
Results may differ from the reference program's by a relative error of at most 0.008.
Values may be sent and summed in bfloat16 or wider, within the bound.
A program may use at most 128 MiB of HBM per device.

```python
import jax
import jax.numpy as jnp
from jax import lax

D = 2048
FF = 7168
TOP = 2
SPLIT = 4
TOK_DEV = 128
EXPERTS = 4
CAP = 80
TOKENS = 2048
N_EP = 16


def draw_expert_ids(key, part):
    key_shift = jax.random.fold_in(key, 11)
    key_offset = jax.random.fold_in(key, 12)
    key_order = jax.random.fold_in(key, 13)
    key_swap = jax.random.fold_in(key, 14)
    shift = jax.random.randint(key_shift, (), 0, EXPERTS)
    blocks = jnp.arange(N_EP, dtype=jnp.int32)
    favoured = ((blocks + shift) % EXPERTS)[:, None]
    positions = jnp.arange(TOK_DEV, dtype=jnp.int32)
    chosen = positions < CAP
    picks_before = jnp.where(chosen, positions, CAP + 2 * (positions - CAP))[None, :]
    offsets = jax.random.randint(key_offset, (N_EP, 1), 0, EXPERTS - 1)
    first_other = (picks_before + offsets) % (EXPERTS - 1)
    second_other = (picks_before + 1 + offsets) % (EXPERTS - 1)
    first_expert = (favoured + 1 + first_other) % EXPERTS
    second_expert = (favoured + 1 + second_other) % EXPERTS
    column_one = jnp.where(chosen[None, :], favoured, first_expert)
    column_two = jnp.where(chosen[None, :], first_expert, second_expert)
    orders = jax.vmap(lambda k: jax.random.permutation(k, TOK_DEV))(jax.random.split(key_order, N_EP))
    column_one = jnp.take_along_axis(column_one, orders, axis=1)
    column_two = jnp.take_along_axis(column_two, orders, axis=1)
    flips = jax.random.randint(key_swap, (N_EP, TOK_DEV), 0, 2)
    left = jnp.where(flips == 1, column_two, column_one)
    right = jnp.where(flips == 1, column_one, column_two)
    paired = jnp.stack([left, right], axis=2)
    return paired.reshape(TOKENS, TOP).astype(jnp.int32)


def steps_of(own_key, extent, shards, low, high):
    level = 1.0
    for position, shards_of in shards:
        heights = jax.random.uniform(jax.random.fold_in(jax.random.fold_in(own_key, 6), position), (shards_of,), jnp.float32, low / len(shards), high / len(shards))
        level = level * jnp.repeat(jnp.exp(heights), extent[position] // shards_of).reshape((-1,) + (1,) * (len(extent) - 1 - position))
    return level


def scatter_about(stream_key, dims, spread, most, pieces=(), kind=jnp.bfloat16):
    entries = spread * jax.random.normal(stream_key, dims, jnp.float32)
    if pieces:
        entries = entries * steps_of(stream_key, dims, pieces, -0.22, 0.18)
    return jnp.clip(entries, -most, most).astype(kind)


def setup_inputs(seed: int = 0, part: int = 0) -> dict:
    key_of = jax.random.split(jax.random.key(seed), 8)
    own_keys = jax.random.split(jax.random.fold_in(key_of[7], part), 8)
    return {
        "tokens": scatter_about(own_keys[0], (TOKENS, D), 1.0, 6.0, ((0, 16),)),
        "norm_gain": jnp.clip(1.0 + 0.18 * jax.random.normal(key_of[1], (D,), jnp.float32), 0.1, 1.9),
        "expert_ids": draw_expert_ids(jax.random.fold_in(jax.random.fold_in(key_of[7], part), 71), part),
        "mix_weights": jnp.clip(0.2 + 0.8 * jax.random.uniform(own_keys[3], (TOKENS, TOP), jnp.float32) ** steps_of(own_keys[3], (TOKENS, TOP), ((0, 16),), -0.2, 0.2), 0.2, 1.0),
        "gate_weight": scatter_about(key_of[4], (D, EXPERTS * FF), D ** -0.5, 0.125, ((1, 16),)),
        "up_weight": scatter_about(key_of[5], (D, EXPERTS * FF), D ** -0.5, 0.125, ((1, 16),)),
        "down_weight": scatter_about(key_of[6], (EXPERTS * FF, D), FF ** -0.5, 0.0625, ((0, 16),)),
    }


def block_slots(ids):
    flat = ids.reshape(-1)
    onehot = (flat[:, None] == jnp.arange(EXPERTS, dtype=jnp.int32)[None, :]).astype(jnp.int32)
    before = jnp.cumsum(onehot, axis=0) - onehot
    return lax.optimization_barrier(jnp.sum(before * onehot, axis=1)).reshape(ids.shape)

def reference(tokens, norm_gain, expert_ids, mix_weights, gate_weight, up_weight, down_weight):
    values = tokens.astype(jnp.float32)
    normed = (values * lax.rsqrt(lax.optimization_barrier(jnp.mean(values * values, axis=-1, keepdims=True)) + 1e-06) * norm_gain).astype(jnp.bfloat16)
    ids = expert_ids.reshape(N_EP, TOK_DEV, TOP)
    slots = jax.vmap(block_slots)(ids)
    source = jnp.broadcast_to(jnp.arange(N_EP, dtype=jnp.int32)[:, None, None], ids.shape)
    rows = jnp.broadcast_to(normed.reshape(N_EP, TOK_DEV, 1, D), (N_EP, TOK_DEV, TOP, D))
    buffers = jnp.zeros((EXPERTS, N_EP, CAP, D), jnp.bfloat16)
    buffers = buffers.at[ids, source, slots].set(rows)
    slice_width = FF // SPLIT

    def one_expert(args):
        expert, block = args
        inputs = block.reshape(N_EP * CAP, D)
        total = jnp.zeros((N_EP * CAP, D), jnp.float32)
        for part in range(SPLIT):
            start = (expert * FF + part * slice_width).astype(jnp.int32)
            w_gate = lax.dynamic_slice_in_dim(gate_weight, start, slice_width, 1)
            w_up = lax.dynamic_slice_in_dim(up_weight, start, slice_width, 1)
            w_down = lax.dynamic_slice_in_dim(down_weight, start, slice_width, 0)
            gate = jnp.dot(inputs, w_gate, preferred_element_type=jnp.float32)
            upper = jnp.dot(inputs, w_up, preferred_element_type=jnp.float32)
            hidden = (jax.nn.silu(gate) * upper).astype(jnp.bfloat16)
            partial_out = jnp.dot(hidden, w_down, preferred_element_type=jnp.float32).astype(jnp.bfloat16)
            total = total + partial_out.astype(jnp.float32)
        return total.reshape(N_EP, CAP, D)
    expert_out = lax.map(one_expert, (jnp.arange(EXPERTS, dtype=jnp.int32), buffers))
    picked = expert_out[ids, source, slots]
    mixed = lax.optimization_barrier(jnp.sum(mix_weights.reshape(N_EP, TOK_DEV, TOP, 1) * picked, axis=2))
    return mixed.reshape(TOKENS, D).astype(jnp.bfloat16)
```

```python
import functools

import jax
import jax.numpy as jnp
from jax import lax
from jax.experimental import pallas as pl
from jax.experimental.pallas import tpu as pltpu
from jax.sharding import PartitionSpec as P

SPLIT = 4
f32, bf16 = jnp.float32, jnp.bfloat16


def tile_of(extent, most):
    tile = most
    while extent % tile:
        tile //= 2
    return tile


def kernel(
    experts,
    tok_ref, gain_ref, ids_ref, mix_ref, wg_hbm, wu_hbm, wd_hbm,
    out_ref,
    wg, wu, wd, normed, disp, xin, hid, part, r1, r2s, r2r, r3s, home, acc,
    w_sem, zs_sem, zr_sem, ys_sem, yr_sem, cs_sem, cr_sem, ds_sem, dr_sem,
    r1s_sem, r1r_sem, r2s_sem, r2r_sem, r3s_sem, r3r_sem,
):
    me = lax.axis_index("ep")
    z = me // SPLIT
    y = (me // 2) % 2
    c = me % 2
    rows, width = tok_ref.shape
    cap = disp.shape[1]
    ff = wg.shape[1]
    top = ids_ref.shape[1]
    at_y = {"ep": z * SPLIT + (1 - y) * 2 + c}
    at_c = {"ep": z * SPLIT + y * 2 + (1 - c)}
    mine = c * 2 + y
    other_y = c * 2 + 1 - y

    def peer(i):
        return z ^ i

    def at_z(i):
        return {"ep": peer(i) * SPLIT + y * 2 + c}

    def remote(src, dst, send, recv, where):
        return pltpu.make_async_remote_copy(
            src_ref=src, dst_ref=dst, send_sem=send, recv_sem=recv,
            device_id=where, device_id_type=pl.DeviceIdType.MESH,
        )

    ft = tile_of(ff, 256)
    nf = ff // ft
    dt = tile_of(width, 256)
    nd = width // dt

    def weight_gu(j):
        cols = pl.ds(pl.multiple_of(j * ft, ft), ft)
        return (
            pltpu.make_async_copy(wg_hbm.at[:, cols], wg.at[:, cols], w_sem.at[0, j]),
            pltpu.make_async_copy(wu_hbm.at[:, cols], wu.at[:, cols], w_sem.at[1, j]),
        )

    weight_d = pltpu.make_async_copy(wd_hbm, wd, w_sem.at[2, 0])

    barrier = pltpu.get_barrier_semaphore()
    for i in range(1, experts):
        pl.semaphore_signal(barrier, inc=1, device_id=at_z(i), device_id_type=pl.DeviceIdType.MESH)
    pl.semaphore_signal(barrier, inc=1, device_id=at_y, device_id_type=pl.DeviceIdType.MESH)
    pl.semaphore_signal(barrier, inc=1, device_id=at_c, device_id_type=pl.DeviceIdType.MESH)

    for j in range(nf):
        for copy in weight_gu(j):
            copy.start()
    weight_d.start()

    step = tile_of(rows, 16)

    @pl.loop(0, rows // step)
    def _(r):
        at = pl.ds(pl.multiple_of(r * step, step), step)
        values = tok_ref[at, :].astype(f32)
        scale = lax.rsqrt(jnp.mean(values * values, axis=-1, keepdims=True) + 1e-06)
        normed[at, :] = (values * scale * gain_ref[...]).astype(bf16)

    lanes = 128
    lane = lax.broadcasted_iota(jnp.int32, (rows, lanes), 1)
    named = ids_ref[:, 0:1] == lane
    for k in range(1, top):
        named = named | (ids_ref[:, k : k + 1] == lane)
    named = named.astype(f32).astype(bf16)
    first = lax.broadcasted_iota(jnp.int32, (rows, rows), 0)
    second = lax.broadcasted_iota(jnp.int32, (rows, rows), 1)
    upper = (first < second).astype(f32).astype(bf16)
    lower = (second < first).astype(f32).astype(bf16)
    eye = (second == first).astype(f32).astype(bf16)
    over_rows = (((0,), (0,)), ((), ()))
    rank_t = lax.dot_general(named, upper, over_rows, preferred_element_type=f32)
    named_t = lax.dot_general(named, eye, over_rows, preferred_element_type=f32)
    rank_t = jnp.where(named_t > 0.5, rank_t, -1.0)
    rank = jnp.dot(lower, named, preferred_element_type=f32)
    rank = jnp.where(named.astype(f32) > 0.5, rank, -1.0)
    expert_row = lax.broadcasted_iota(jnp.int32, (lanes, rows), 0)

    def dispatch(e, dst):
        slot = jnp.sum(jnp.where(expert_row == e, rank_t, 0.0), axis=0, keepdims=True)
        place = lax.broadcasted_iota(jnp.int32, (cap, rows), 0)
        pick = (place == slot.astype(jnp.int32)).astype(f32).astype(bf16)
        wide = tile_of(width, 512)
        for n in range(width // wide):
            cols = slice(n * wide, (n + 1) * wide)
            dst[:, cols] = jnp.dot(pick, normed[:, cols], preferred_element_type=f32).astype(bf16)

    def z_copy(i):
        return remote(disp.at[i], xin.at[z, mine], zs_sem.at[i], zr_sem.at[z], at_z(i))

    def z_arrival(i):
        return remote(disp.at[i], xin.at[peer(i), mine], zs_sem.at[i], zr_sem.at[peer(i)], at_z(i))

    def y_copy(i):
        slot = xin.at[peer(i), mine]
        return remote(slot, slot, ys_sem.at[i], yr_sem.at[i], at_y)

    def y_arrival(i):
        slot = xin.at[peer(i), other_y]
        return remote(slot, slot, ys_sem.at[i], yr_sem.at[i], at_y)

    def c_copy(i):
        slot = xin.at[peer(i), mine]
        return remote(slot, slot, cs_sem.at[i], cr_sem.at[i], at_c)

    def c_arrival(i):
        slot = xin.at[peer(i), (1 - c) * 2 + y]
        return remote(slot, slot, cs_sem.at[i], cr_sem.at[i], at_c)

    def d_copy(i):
        slot = xin.at[peer(i), other_y]
        return remote(slot, slot, ds_sem.at[i], dr_sem.at[i], at_c)

    def d_arrival(i):
        slot = xin.at[peer(i), (1 - c) * 2 + 1 - y]
        return remote(slot, slot, ds_sem.at[i], dr_sem.at[i], at_c)

    def r1_copy(i):
        return remote(part.at[i, 1 - c], r1.at[i], r1s_sem.at[i], r1r_sem.at[i], at_c)

    def r2_copy(i):
        return remote(r2s.at[i], r2r.at[i], r2s_sem.at[i], r2r_sem.at[i], at_y)

    def r3_copy(i):
        return remote(r3s.at[i], home.at[z], r3s_sem.at[i], r3r_sem.at[z], at_z(i))

    def r3_arrival(i):
        return remote(r3s.at[i], home.at[peer(i)], r3s_sem.at[i], r3r_sem.at[peer(i)], at_z(i))

    dispatch(z, xin.at[z, mine])
    pl.semaphore_wait(barrier, experts + 1)
    y_copy(0).start()
    c_copy(0).start()

    @pl.loop(1, experts)
    def _(i):
        dispatch(peer(i), disp.at[i])
        z_copy(i).start()

    acc[...] = jnp.zeros_like(acc)

    def gate_up(i, low, high):
        @pl.loop(low, high)
        def _(j):
            @pl.when(i == 0)
            def _():
                for copy in weight_gu(j):
                    copy.wait()

            cols = pl.ds(pl.multiple_of(j * ft, ft), ft)
            inputs = xin[peer(i)].reshape(SPLIT * cap, width)
            gate = jnp.dot(inputs, wg[:, cols], preferred_element_type=f32)
            up = jnp.dot(inputs, wu[:, cols], preferred_element_type=f32)
            hid[:, cols] = (gate / (1.0 + jnp.exp(-gate)) * up).astype(bf16)

    def down(i):
        @pl.when(i == 0)
        def _():
            weight_d.wait()

        @pl.loop(0, nd)
        def _(j):
            cols = pl.ds(pl.multiple_of(j * dt, dt), dt)
            res = jnp.dot(hid[...], wd[:, cols], preferred_element_type=f32).astype(bf16)
            part[i, :, :, :, cols] = res.reshape(2, 2, cap, dt)

    def reduce_chip(i):
        r1_copy(i).wait_recv()

        @pl.loop(0, cap // 16)
        def _(r):
            at = pl.ds(pl.multiple_of(r * 16, 16), 16)
            r2s[i, at, :] = (
                part[i, c, 1 - y, at, :].astype(f32) + r1[i, 1 - y, at, :].astype(f32)
            ).astype(bf16)

        r2_copy(i).start()

    def reduce_group(i):
        r2_copy(i).wait_recv()

        def total(at):
            return (
                part[i, c, y, at, :].astype(f32)
                + r1[i, y, at, :].astype(f32)
                + r2r[i, at, :].astype(f32)
            ).astype(bf16)

        @pl.loop(0, cap // 16)
        def _(r):
            at = pl.ds(pl.multiple_of(r * 16, 16), 16)

            @pl.when(i == 0)
            def _():
                home[z, at, :] = total(at)

            @pl.when(i > 0)
            def _():
                r3s[i, at, :] = total(at)

        @pl.when(i > 0)
        def _():
            r3_copy(i).start()

    @pl.loop(0, experts)
    def _(i):
        y_arrival(i).wait_recv()
        d_copy(i).start()
        c_arrival(i).wait_recv()
        d_arrival(i).wait_recv()
        half = (nf + 1) // 2
        gate_up(i, 0, half)

        @pl.when(i + 1 < experts)
        def _():
            z_arrival(i + 1).wait_recv()
            y_copy(i + 1).start()
            c_copy(i + 1).start()

        gate_up(i, half, nf)

        @pl.when(i > 0)
        def _():
            reduce_chip(i - 1)

        down(i)
        r1_copy(i).start()

        @pl.when(i > 0)
        def _():
            reduce_group(i - 1)

    reduce_chip(experts - 1)
    reduce_group(experts - 1)

    @pl.loop(0, experts)
    def _(i):
        e = peer(i)

        @pl.when(i > 0)
        def _():
            r3_arrival(i).wait_recv()

        slot = jnp.sum(jnp.where(lane == e, rank, 0.0), axis=1, keepdims=True)
        place = lax.broadcasted_iota(jnp.int32, (rows, cap), 1)
        pick = (place == slot.astype(jnp.int32)).astype(f32).astype(bf16)
        weight = jnp.where(ids_ref[:, 0:1] == e, mix_ref[:, 0:1], 0.0)
        for k in range(1, top):
            weight = weight + jnp.where(ids_ref[:, k : k + 1] == e, mix_ref[:, k : k + 1], 0.0)
        wide = tile_of(width, 512)
        for n in range(width // wide):
            cols = slice(n * wide, (n + 1) * wide)
            acc[:, cols] += weight * jnp.dot(pick, home[e, :, cols], preferred_element_type=f32)

    out_ref[...] = acc[...].astype(bf16)

    @pl.loop(0, experts)
    def _(i):
        @pl.when(i > 0)
        def _():
            z_copy(i).wait_send()
            r3_copy(i).wait_send()

        y_copy(i).wait_send()
        c_copy(i).wait_send()
        d_copy(i).wait_send()
        r1_copy(i).wait_send()
        r2_copy(i).wait_send()


def local(tokens, norm_gain, expert_ids, mix_weights, gate_weight, up_weight, down_weight):
    n_dev = lax.axis_size("ep")
    experts = n_dev // SPLIT
    rows, width = tokens.shape
    top = expert_ids.shape[1]
    ff = gate_weight.shape[1]
    cap = (rows * top * SPLIT * 5 + 4 * n_dev - 1) // (4 * n_dev)
    cap = (cap + 15) // 16 * 16
    nf = ff // tile_of(ff, 256)
    dma = pltpu.SemaphoreType.DMA
    vmem = pl.BlockSpec(memory_space=pltpu.VMEM)
    hbm = pl.BlockSpec(memory_space=pl.ANY)
    block = (cap, width)
    return pl.pallas_call(
        functools.partial(kernel, experts),
        out_shape=jax.ShapeDtypeStruct((rows, width), bf16),
        in_specs=[vmem, vmem, vmem, vmem, hbm, hbm, hbm],
        out_specs=vmem,
        scratch_shapes=[
            pltpu.VMEM((width, ff), bf16),
            pltpu.VMEM((width, ff), bf16),
            pltpu.VMEM((ff, width), bf16),
            pltpu.VMEM((rows, width), bf16),
            pltpu.VMEM((experts,) + block, bf16),
            pltpu.VMEM((experts, SPLIT) + block, bf16),
            pltpu.VMEM((SPLIT * cap, ff), bf16),
            pltpu.VMEM((experts, 2, 2) + block, bf16),
            pltpu.VMEM((experts, 2) + block, bf16),
            pltpu.VMEM((experts,) + block, bf16),
            pltpu.VMEM((experts,) + block, bf16),
            pltpu.VMEM((experts,) + block, bf16),
            pltpu.VMEM((experts,) + block, bf16),
            pltpu.VMEM((rows, width), f32),
            dma((3, nf)),
        ] + [dma((experts,))] * 14,
        compiler_params=pltpu.CompilerParams(
            collective_id=0, has_side_effects=True, vmem_limit_bytes=64 * 1024 * 1024 - 65536,
        ),
    )(tokens, norm_gain.reshape(1, width), expert_ids, mix_weights, gate_weight, up_weight, down_weight)


def solution(mesh):
    in_specs = (
        P(("grp", "ep"), None),
        P(),
        P(("grp", "ep"), None),
        P(("grp", "ep"), None),
        P(None, "ep"),
        P(None, "ep"),
        P("ep", None),
    )
    out_specs = P(("grp", "ep"), None)
    return jax.shard_map(local, mesh=mesh, in_specs=in_specs, out_specs=out_specs, check_vma=False)
```

```python
import functools

import jax
import jax.numpy as jnp
from jax import lax
from jax.experimental import pallas as pl
from jax.experimental.pallas import tpu as pltpu
from jax.sharding import PartitionSpec as P

SPLIT = 4
CHUNK = 16
f32, bf16 = jnp.float32, jnp.bfloat16


def tile_of(extent, most):
    tile = most
    while extent % tile:
        tile //= 2
    return tile


def kernel(
    experts,
    tok_ref, gain_ref, ids_ref, mix_ref, wg_hbm, wu_hbm, wd_hbm,
    out_ref,
    wg, wu, wd, normed, disp, xin, hid, part, r1, r2s, r2r, r3s, home, acc,
    w_sem, zs_sem, zr_sem, ys_sem, yr_sem, cs_sem, cr_sem, ds_sem, dr_sem,
    r1s_sem, r1r_sem, r2s_sem, r2r_sem, r3s_sem, r3r_sem,
):
    me = lax.axis_index("ep")
    z = me // SPLIT
    y = (me // 2) % 2
    c = me % 2
    rows, width = tok_ref.shape
    cap = disp.shape[1]
    nq = cap // CHUNK
    ff = wg.shape[1]
    top = ids_ref.shape[0]
    at_y = {"ep": z * SPLIT + (1 - y) * 2 + c}
    at_c = {"ep": z * SPLIT + y * 2 + (1 - c)}
    mine = c * 2 + y
    other_y = c * 2 + 1 - y
    other_c = (1 - c) * 2 + y
    other_yc = (1 - c) * 2 + 1 - y

    def peer(k):
        shift = jnp.where(k == 0, 0, (k + experts // 2 - 2) % (experts - 1) + 1)
        return z ^ shift

    def at_z(k):
        return {"ep": peer(k) * SPLIT + y * 2 + c}

    def remote(src, dst, send, recv, where):
        return pltpu.make_async_remote_copy(
            src_ref=src, dst_ref=dst, send_sem=send, recv_sem=recv,
            device_id=where, device_id_type=pl.DeviceIdType.MESH,
        )

    def chunk(q):
        return pl.ds(pl.multiple_of(q * CHUNK, CHUNK), CHUNK)

    ft = tile_of(ff, 256)
    nf = ff // ft
    dt = tile_of(width, 256)
    nd = width // dt

    def weight_gu(j):
        cols = pl.ds(pl.multiple_of(j * ft, ft), ft)
        return (
            pltpu.make_async_copy(wg_hbm.at[:, cols], wg.at[:, cols], w_sem.at[0, j]),
            pltpu.make_async_copy(wu_hbm.at[:, cols], wu.at[:, cols], w_sem.at[1, j]),
        )

    weight_d = pltpu.make_async_copy(wd_hbm, wd, w_sem.at[2, 0])

    barrier = pltpu.get_barrier_semaphore()

    for k in range(1, experts):
        pl.semaphore_signal(barrier, inc=1, device_id=at_z(k), device_id_type=pl.DeviceIdType.MESH)
    pl.semaphore_signal(barrier, inc=1, device_id=at_y, device_id_type=pl.DeviceIdType.MESH)
    pl.semaphore_signal(barrier, inc=1, device_id=at_c, device_id_type=pl.DeviceIdType.MESH)

    for j in range(nf):
        for copy in weight_gu(j):
            copy.start()
    weight_d.start()

    step = tile_of(rows, 16)

    @pl.loop(0, rows // step)
    def _(r):
        at = pl.ds(pl.multiple_of(r * step, step), step)
        values = tok_ref[at, :].astype(f32)
        scale = lax.rsqrt(jnp.mean(values * values, axis=-1, keepdims=True) + 1e-06)
        normed[at, :] = (values * scale * gain_ref[...]).astype(bf16)

    lanes = 128
    expert_row = lax.broadcasted_iota(jnp.int32, (lanes, rows), 0)
    named = ids_ref[0:1, :] == expert_row
    weight_t = jnp.where(named, mix_ref[0:1, :], 0.0)
    for k in range(1, top):
        hit = ids_ref[k : k + 1, :] == expert_row
        named = named | hit
        weight_t = weight_t + jnp.where(hit, mix_ref[k : k + 1, :], 0.0)
    named = named.astype(f32)
    first = lax.broadcasted_iota(jnp.int32, (rows, rows), 0)
    second = lax.broadcasted_iota(jnp.int32, (rows, rows), 1)
    upper = (first < second).astype(f32).astype(bf16)
    rank_t = jnp.dot(named.astype(bf16), upper, preferred_element_type=f32)
    rank_t = jnp.where(named > 0.5, rank_t, -1.0)
    rank = jnp.transpose(rank_t)
    weight_c = jnp.transpose(weight_t)
    lane = lax.broadcasted_iota(jnp.int32, (rows, lanes), 1)

    def dispatch(e, dst):
        slot = jnp.sum(jnp.where(expert_row == e, rank_t, 0.0), axis=0, keepdims=True)
        place = lax.broadcasted_iota(jnp.int32, (cap, rows), 0)
        pick = (place == slot.astype(jnp.int32)).astype(f32).astype(bf16)
        wide = tile_of(width, 512)
        for n in range(width // wide):
            cols = slice(n * wide, (n + 1) * wide)
            dst[:, cols] = jnp.dot(pick, normed[:, cols], preferred_element_type=f32).astype(bf16)

    def z_copy(k, q):
        return remote(disp.at[k, chunk(q)], xin.at[z, mine, chunk(q)], zs_sem.at[k, q], zr_sem.at[z, q], at_z(k))

    def z_arrival(k, q):
        p = peer(k)
        return remote(disp.at[k, chunk(q)], xin.at[p, mine, chunk(q)], zs_sem.at[k, q], zr_sem.at[p, q], at_z(k))

    def in_group(sub, send, recv, where):
        def make(k, q):
            slot = xin.at[peer(k), sub, chunk(q)]
            return remote(slot, slot, send.at[k, q], recv.at[k, q], where)

        return make

    y_copy = in_group(mine, ys_sem, yr_sem, at_y)
    y_arrival = in_group(other_y, ys_sem, yr_sem, at_y)
    c_copy = in_group(mine, cs_sem, cr_sem, at_c)
    c_arrival = in_group(other_c, cs_sem, cr_sem, at_c)
    d_copy = in_group(other_y, ds_sem, dr_sem, at_c)
    d_arrival = in_group(other_yc, ds_sem, dr_sem, at_c)

    def r1_copy(k, v, q):
        return remote(
            part.at[k, 1 - c, v, chunk(q)], r1.at[k, v, chunk(q)], r1s_sem.at[k, v, q], r1r_sem.at[k, v, q], at_c
        )

    def r2_copy(k, q):
        return remote(r2s.at[k, chunk(q)], r2r.at[k, chunk(q)], r2s_sem.at[k, q], r2r_sem.at[k, q], at_y)

    def r3_copy(k, q):
        return remote(r3s.at[k, chunk(q)], home.at[z, chunk(q)], r3s_sem.at[k, q], r3r_sem.at[z, q], at_z(k))

    def r3_arrival(k, q):
        p = peer(k)
        return remote(r3s.at[k, chunk(q)], home.at[p, chunk(q)], r3s_sem.at[k, q], r3r_sem.at[p, q], at_z(k))

    def forward_z(k, q):
        @pl.when(k > 0)
        def _():
            z_arrival(k, q).wait_recv()

        y_copy(k, q).start()
        c_copy(k, q).start()

    def forward_y(k, q):
        y_arrival(k, q).wait_recv()
        d_copy(k, q).start()

    def reduce_chip(k, q):
        at = chunk(q)
        r1_copy(k, 1 - y, q).wait_recv()
        r2s[k, at, :] = (part[k, c, 1 - y, at, :].astype(f32) + r1[k, 1 - y, at, :].astype(f32)).astype(bf16)
        r2_copy(k, q).start()

    def reduce_group(k, q):
        @pl.when(q < nq)
        def _():
            at = chunk(q)
            r1_copy(k, y, q).wait_recv()
            r2_copy(k, q).wait_recv()
            total = (
                part[k, c, y, at, :].astype(f32) + r1[k, y, at, :].astype(f32) + r2r[k, at, :].astype(f32)
            ).astype(bf16)

            @pl.when(k == 0)
            def _():
                home[z, at, :] = total

            @pl.when(k > 0)
            def _():
                r3s[k, at, :] = total
                r3_copy(k, q).start()

    dispatch(z, xin.at[z, mine])
    pl.semaphore_wait(barrier, experts + 1)

    @pl.loop(0, nq)
    def _(q):
        forward_z(0, q)

    @pl.loop(1, experts)
    def _(k):
        dispatch(peer(k), disp.at[k])

        @pl.loop(0, nq)
        def _(q):
            z_copy(k, q).start()

    acc[...] = jnp.zeros_like(acc)

    def gate_up(k, j):
        @pl.when(k == 0)
        def _():
            for copy in weight_gu(j):
                copy.wait()

        cols = pl.ds(pl.multiple_of(j * ft, ft), ft)
        inputs = xin[peer(k)].reshape(SPLIT * cap, width)
        gate = jnp.dot(inputs, wg[:, cols], preferred_element_type=f32)
        up = jnp.dot(inputs, wu[:, cols], preferred_element_type=f32)
        hid[:, cols] = (gate / (1.0 + jnp.exp(-gate)) * up).astype(bf16)

    def down(k, j):
        cols = pl.ds(pl.multiple_of(j * dt, dt), dt)
        res = jnp.dot(hid[...], wd[:, cols], preferred_element_type=f32).astype(bf16)
        part[k, :, :, :, cols] = res.reshape(2, 2, cap, dt)

    early = 2

    @pl.loop(0, nq)
    def _(q):
        forward_y(0, q)

        @pl.when(q < early)
        def _():
            forward_z(1, q)

    @pl.loop(0, experts)
    def _(k):
        @pl.loop(0, nq)
        def _(q):
            c_arrival(k, q).wait_recv()

        @pl.loop(0, nq)
        def _(q):
            d_arrival(k, q).wait_recv()

        @pl.loop(0, max(nf, nq))
        def _(j):
            @pl.when(j < nf)
            def _():
                gate_up(k, j)

            @pl.when((j < nq) & (k + 1 < experts) & ((k > 0) | (j >= early)))
            def _():
                forward_z(k + 1, j)

            @pl.when((j < nq) & (k > 0))
            def _():
                reduce_chip(k - 1, j)

        @pl.when(k == 0)
        def _():
            weight_d.wait()

        @pl.loop(0, max(nd, nq))
        def _(j):
            @pl.when(j < nd)
            def _():
                down(k, j)

            @pl.when((j < nq) & (k + 1 < experts))
            def _():
                forward_y(k + 1, j)

            @pl.when((j < nq) & (k > 0))
            def _():
                reduce_group(k - 1, j)

        for side in (1 - y, y):

            @pl.loop(0, nq)
            def _(q):
                r1_copy(k, side, q).start()

    @pl.loop(0, nq)
    def _(q):
        reduce_chip(experts - 1, q)

    @pl.loop(0, nq)
    def _(q):
        reduce_group(experts - 1, q)

    @pl.loop(0, experts)
    def _(k):
        e = peer(k)

        @pl.when(k > 0)
        def _():
            @pl.loop(0, nq)
            def _(q):
                r3_arrival(k, q).wait_recv()

        slot = jnp.sum(jnp.where(lane == e, rank, 0.0), axis=1, keepdims=True)
        weight = jnp.sum(jnp.where(lane == e, weight_c, 0.0), axis=1, keepdims=True)
        place = lax.broadcasted_iota(jnp.int32, (rows, cap), 1)
        pick = (place == slot.astype(jnp.int32)).astype(f32).astype(bf16)
        wide = tile_of(width, 512)
        for n in range(width // wide):
            cols = slice(n * wide, (n + 1) * wide)
            acc[:, cols] += weight * jnp.dot(pick, home[e, :, cols], preferred_element_type=f32)

    out_ref[...] = acc[...].astype(bf16)

    @pl.loop(0, experts)
    def _(k):
        @pl.when(k > 0)
        def _():
            @pl.loop(0, nq)
            def _(q):
                z_copy(k, q).wait_send()

            @pl.loop(0, nq)
            def _(q):
                r3_copy(k, q).wait_send()

        @pl.loop(0, nq)
        def _(q):
            y_copy(k, q).wait_send()
            c_copy(k, q).wait_send()

        @pl.loop(0, nq)
        def _(q):
            d_copy(k, q).wait_send()
            r2_copy(k, q).wait_send()

        for v in range(2):
            @pl.loop(0, nq)
            def _(q):
                r1_copy(k, v, q).wait_send()


def local(tokens, norm_gain, expert_ids, mix_weights, gate_weight, up_weight, down_weight):
    n_dev = lax.axis_size("ep")
    experts = n_dev // SPLIT
    rows, width = tokens.shape
    top = expert_ids.shape[1]
    ff = gate_weight.shape[1]
    cap = (rows * top * SPLIT * 5 + 4 * n_dev - 1) // (4 * n_dev)
    cap = (cap + CHUNK - 1) // CHUNK * CHUNK
    nq = cap // CHUNK
    nf = ff // tile_of(ff, 256)
    dma = pltpu.SemaphoreType.DMA
    vmem = pl.BlockSpec(memory_space=pltpu.VMEM)
    hbm = pl.BlockSpec(memory_space=pl.ANY)
    block = (cap, width)
    return pl.pallas_call(
        functools.partial(kernel, experts),
        out_shape=jax.ShapeDtypeStruct((rows, width), bf16),
        in_specs=[vmem, vmem, vmem, vmem, hbm, hbm, hbm],
        out_specs=vmem,
        scratch_shapes=[
            pltpu.VMEM((width, ff), bf16),
            pltpu.VMEM((width, ff), bf16),
            pltpu.VMEM((ff, width), bf16),
            pltpu.VMEM((rows, width), bf16),
            pltpu.VMEM((experts,) + block, bf16),
            pltpu.VMEM((experts, SPLIT) + block, bf16),
            pltpu.VMEM((SPLIT * cap, ff), bf16),
            pltpu.VMEM((experts, 2, 2) + block, bf16),
            pltpu.VMEM((experts, 2) + block, bf16),
            pltpu.VMEM((experts,) + block, bf16),
            pltpu.VMEM((experts,) + block, bf16),
            pltpu.VMEM((experts,) + block, bf16),
            pltpu.VMEM((experts,) + block, bf16),
            pltpu.VMEM((rows, width), f32),
            dma((3, nf)),
        ] + [dma((experts, nq))] * 8 + [dma((experts, 2, nq))] * 2 + [dma((experts, nq))] * 4,
        compiler_params=pltpu.CompilerParams(
            collective_id=0, has_side_effects=True, vmem_limit_bytes=64 * 1024 * 1024 - 65536,
        ),
    )(tokens, norm_gain.reshape(1, width), expert_ids.T, mix_weights.T, gate_weight, up_weight, down_weight)


def solution(mesh):
    in_specs = (
        P(("grp", "ep"), None),
        P(),
        P(("grp", "ep"), None),
        P(("grp", "ep"), None),
        P(None, "ep"),
        P(None, "ep"),
        P("ep", None),
    )
    out_specs = P(("grp", "ep"), None)
    return jax.shard_map(local, mesh=mesh, in_specs=in_specs, out_specs=out_specs, check_vma=False)
```
